32 devices in a mesh: grp: 2 (over y), fs: 4 (over z), tp: 4 (over x, core).
Axes of the slice: x: 2, y: 2, z: 4, core: 2. Of those that a mesh axis runs over, the one named last changes fastest.
Arguments:
- tokens: bfloat16 [4096, 2048], P(('grp', 'fs', 'tp')), parts along dimension 0, may hold values from -6 to 6
- route_ids: int32 [4096, 8], P(('grp', 'fs', 'tp')), parts along dimension 0, may hold values from 0 to 15, all different within a row; in each aligned block of 128 rows (0 to 127, 128 to 255, ...) at most 96 rows name the same one
- route_scores: float32 [4096, 8], P(('grp', 'fs', 'tp')), parts along dimension 0, may hold values from 0.05 to 1
- norm_gain: float32 [2048], P('fs'), may hold values from 0.1 to 1.9
- expert_gate: float32 [16, 2048, 256], P(None, 'fs', 'tp'), may hold values from -0.125 to 0.125
- expert_up: float32 [16, 2048, 256], P(None, 'fs', 'tp'), may hold values from -0.125 to 0.125
- expert_down: float32 [16, 256, 2048], P(None, 'fs', 'tp'), may hold values from -0.375 to 0.375
- shared_gate: float32 [2048, 256], P('fs', 'tp'), may hold values from -0.125 to 0.125
- shared_up: float32 [2048, 256], P('fs', 'tp'), may hold values from -0.125 to 0.125
- shared_down: float32 [256, 2048], P('fs', 'tp'), may hold values from -0.375 to 0.375
Outputs:
- mixed: bfloat16 [4096, 2048], P(('grp', 'fs', 'tp')), parts along dimension 0
- sampler_gate: bfloat16 [32, 2048, 256], P(('grp', 'fs', 'tp')), parts along dimension 0
- sampler_up: bfloat16 [32, 2048, 256], P(('grp', 'fs', 'tp')), parts along dimension 0
- sampler_down: bfloat16 [32, 256, 2048], P(('grp', 'fs', 'tp')), parts along dimension 0
- sampler_shared_gate: bfloat16 [4096, 256], P(('grp', 'fs')), parts along dimension 0
- sampler_shared_up: bfloat16 [4096, 256], P(('grp', 'fs')), parts along dimension 0
- sampler_shared_down: bfloat16 [512, 2048], P(('grp', 'fs')), parts along dimension 0
The draws below stay inside these ranges and needn't reach their ends.
There are 2 independent parts, one for each index of `grp`. The reference program is written for one: setup_inputs(seed, part) draws one part's arguments, and reference() takes and returns one part's arrays. A program takes and returns all parts, laid end to end along the dimension named above; an argument that names none is the same for every part. Nothing has to cross between parts.
Inputs may be any that keep to these rules, and one draw needn't show every extreme that they name: `route_ids`: each row names 8 different experts. Among the 128 rows of one device no expert is named more than 96 times, a bound that some block reaches.
All inputs are finite; a program needn't handle non-finite values.
Results may differ from the reference program's by a relative error of at most 0.0084.
Values may be sent and summed in bfloat16 or wider, within the bound.
No kernel may reach another device: no remote copies, remote signals or barrier semaphores. Data moves between devices by JAX's collectives and lax.ppermute only.
A program may use at most 128 MiB of HBM per device.

```python
import math
import jax
import jax.numpy as jnp
import numpy as np
from jax import lax

D = 2048
F = 256
SH = 256
TOP_K = 8
TOK_DEV = 128
EXPERTS = 16
TOKENS = 2048
CAP = 96


def level_of(rng, extent, pieces, least, largest):
    def one(dim, blocks):
        draws = jax.random.uniform(jax.random.fold_in(jax.random.fold_in(rng, 6), dim), (blocks,), jnp.float32, least / len(pieces), largest / len(pieces))
        return jnp.repeat(jnp.exp(draws), extent[dim] // blocks).reshape((-1,) + (1,) * (len(extent) - dim - 1))

    factor_of = one(*pieces[0])
    for cut in pieces[1:]:
        factor_of = factor_of * one(*cut)
    return factor_of


def routed_block(own_key, own, number, rows, number_of, top, most, skew):
    ranking = jax.random.permutation(own_key, number_of)
    packed, usual = shares(number_of, rows * top, most, skew, True), shares(number_of, rows * top, most, skew, False)
    places = jnp.arange(number_of)

    def named(tallies, rotation):
        used = int((tallies > 0).sum())
        fixed = max(1, used // 4)
        moved = fixed + (places - fixed + rotation * (used - fixed)) % max(1, number_of - fixed)
        return jnp.zeros((number_of,), jnp.int32).at[ranking[jnp.where(places < fixed, places, moved)]].set(jnp.asarray(tallies, jnp.int32))

    tallies = jnp.where(number % 4 == 0, named(packed, number // 4), named(usual, number - number // 4 - 1))
    mixed = jax.random.permutation(jax.random.fold_in(own, 3), number_of)
    giver, taker = mixed[0:number_of // 2 * 2:2], mixed[1:number_of // 2 * 2:2]
    slack = jnp.minimum(tallies[giver] - 1, most - tallies[taker]) // 2
    slack = jnp.where((giver == ranking[0]) | (taker == ranking[0]) | (tallies[taker] == 0), 0, jnp.maximum(slack, 0))
    moved = jax.random.randint(jax.random.fold_in(own, 4), (number_of // 2,), 0, 1 << 20) % (slack + 1)
    tallies = tallies.at[giver].add(-moved).at[taker].add(moved)
    items = jnp.searchsorted(jnp.cumsum(tallies), jnp.arange(rows * top), side="right").astype(jnp.int32)
    listing = items.reshape(top, rows).T
    listing = listing[jax.random.permutation(jax.random.fold_in(own, 1), rows)]
    rotation = jax.random.randint(jax.random.fold_in(own, 2), (rows, 1), 0, top)
    return jnp.take_along_axis(listing, (jnp.arange(top)[None, :] + rotation) % top, axis=1)


def shares(amount, total, most, slope, full):
    weights = [(1 << 20) // math.isqrt(grade ** slope) + 1 for grade in range(1, amount + 1)]
    largest = most if full else min(most, max(-(-total // amount), total * weights[0] // sum(weights)))
    least = 1 if total - largest >= amount - 1 else 0
    given, surplus = [largest] + [least] * (amount - 1), total - largest - least * (amount - 1)
    while surplus > 0:
        movable = [i for i in range(1, amount) if given[i] < largest] or [i for i in range(1, amount) if given[i] < most]
        whole, left = sum([weights[i] for i in movable]), surplus
        for i in movable:
            addition = min(most - given[i], max(1, left * weights[i] // whole), surplus)
            given[i] = given[i] + addition
            surplus = surplus - addition
    return np.array(given)


def bell_draw(stream_key, shape, width, bound, pieces=(), held_as=jnp.bfloat16):
    result = jax.random.normal(stream_key, shape, jnp.float32) * width
    if len(pieces) > 0:
        result = level_of(stream_key, shape, pieces, -0.22, 0.18) * result
    return jnp.clip(result, min=-bound, max=bound).astype(held_as)


def setup_inputs(seed: int = 0, part: int = 0) -> dict:
    arg_keys = jax.random.split(jax.random.key(seed), 11)
    part_keys = jax.random.split(jax.random.fold_in(arg_keys[10], part), 11)
    tokens = bell_draw(part_keys[0], (TOKENS, D), 1.0, 6.0, ((0, 16),))
    route_ids_keys = jax.random.split(jax.random.fold_in(part_keys[1], 1), TOKENS // TOK_DEV)
    route_ids_turns = jax.random.permutation(jax.random.fold_in(part_keys[1], 3), TOKENS // TOK_DEV)
    route_ids = jax.vmap(lambda own, number: routed_block(jax.random.fold_in(part_keys[1], 2), own, number, TOK_DEV, EXPERTS, TOP_K, CAP, 1))(route_ids_keys, route_ids_turns).reshape((TOKENS, TOP_K))
    route_scores = jnp.clip(0.05 + 0.95 * jax.random.uniform(part_keys[2], (TOKENS, TOP_K), jnp.float32) ** level_of(part_keys[2], (TOKENS, TOP_K), ((0, 16),), -0.2, 0.2), 0.05, 1.0)
    norm_gain = jnp.clip(1.0 + 0.18 * jax.random.normal(arg_keys[3], (D,), jnp.float32), 0.1, 1.9)
    expert_gate = bell_draw(arg_keys[4], (EXPERTS, D, F), D ** -0.5, 0.125, ((1, 4), (2, 4)), jnp.float32)
    expert_up = bell_draw(arg_keys[5], (EXPERTS, D, F), D ** -0.5, 0.125, ((1, 4), (2, 4)), jnp.float32)
    expert_down = bell_draw(arg_keys[6], (EXPERTS, F, D), F ** -0.5, 0.375, ((1, 4), (2, 4)), jnp.float32)
    shared_gate = bell_draw(arg_keys[7], (D, SH), D ** -0.5, 0.125, ((0, 4), (1, 4)), jnp.float32)
    shared_up = bell_draw(arg_keys[8], (D, SH), D ** -0.5, 0.125, ((0, 4), (1, 4)), jnp.float32)
    shared_down = bell_draw(arg_keys[9], (SH, D), SH ** -0.5, 0.375, ((0, 4), (1, 4)), jnp.float32)
    return {"tokens": tokens, "route_ids": route_ids, "route_scores": route_scores, "norm_gain": norm_gain, "expert_gate": expert_gate, "expert_up": expert_up, "expert_down": expert_down, "shared_gate": shared_gate, "shared_up": shared_up, "shared_down": shared_down}


EPSILON = 1e-06
route_scale = 2.5

def reference(tokens, route_ids, route_scores, norm_gain, expert_gate, expert_up, expert_down, shared_gate, shared_up, shared_down):
    gain_col = norm_gain[:, None]
    sampler_gate = (gain_col[None] * expert_gate).astype(jnp.bfloat16)
    sampler_up = (gain_col[None] * expert_up).astype(jnp.bfloat16)
    sampler_down = expert_down.astype(jnp.bfloat16)
    sampler_shared_gate = (gain_col * shared_gate).astype(jnp.bfloat16)
    sampler_shared_up = (gain_col * shared_up).astype(jnp.bfloat16)
    sampler_shared_down = shared_down.astype(jnp.bfloat16)
    widened = tokens.astype(jnp.float32)
    normed = (widened * lax.rsqrt(lax.optimization_barrier(jnp.mean(widened * widened, axis=1, keepdims=True)) + EPSILON)).astype(jnp.bfloat16)
    weights = route_scale * route_scores / lax.optimization_barrier(jnp.sum(route_scores, axis=1, keepdims=True))
    gate_part = jnp.dot(normed, sampler_shared_gate, preferred_element_type=jnp.float32)
    up_part = jnp.dot(normed, sampler_shared_up, preferred_element_type=jnp.float32)
    shared_hidden = (jax.nn.silu(gate_part) * up_part).astype(jnp.bfloat16)
    shared_term = jnp.dot(shared_hidden, sampler_shared_down, preferred_element_type=jnp.float32)
    flat_ids = route_ids.reshape(-1)
    flat_weights = weights.reshape(-1)
    slots = EXPERTS * CAP

    def one_expert(expert, totals):
        matches = flat_ids == expert
        picked = jnp.nonzero(matches, size=slots, fill_value=0)[0].astype(jnp.int32)
        filled = (jnp.arange(slots, dtype=jnp.int32) < jnp.sum(matches.astype(jnp.int32))).astype(jnp.float32)
        owners = (picked // TOP_K).astype(jnp.int32)
        row_block = normed[owners]
        w_gate = lax.dynamic_index_in_dim(sampler_gate, expert, 0, keepdims=False)
        w_up = lax.dynamic_index_in_dim(sampler_up, expert, 0, keepdims=False)
        w_down = lax.dynamic_index_in_dim(sampler_down, expert, 0, keepdims=False)
        gate_rows = jnp.dot(row_block, w_gate, preferred_element_type=jnp.float32)
        up_rows = jnp.dot(row_block, w_up, preferred_element_type=jnp.float32)
        hidden = (jax.nn.silu(gate_rows) * up_rows).astype(jnp.bfloat16)
        produced = jnp.dot(hidden, w_down, preferred_element_type=jnp.float32).astype(jnp.bfloat16)
        factor = flat_weights[picked] * filled
        return totals.at[owners].add(produced.astype(jnp.float32) * factor[:, None])
    routed = lax.fori_loop(0, EXPERTS, one_expert, jnp.zeros(tokens.shape, jnp.float32))
    mixed = (routed + shared_term).astype(jnp.bfloat16)
    return (mixed, sampler_gate, sampler_up, sampler_down, sampler_shared_gate, sampler_shared_up, sampler_shared_down)
```

```python
import functools
import math

import jax
import jax.numpy as jnp
from jax import lax
from jax.experimental import pallas as pl
from jax.experimental.pallas import tpu as pltpu
from jax.sharding import PartitionSpec as P

EPSILON = 1e-06
route_scale = 2.5
LANES = 128
PACKED_ROWS = 16
CORES = 2


def ceil_to(value, unit):
    return -(-value // unit) * unit


def expert_rows(row_block, w_gate, w_up, w_down):
    gate_rows = jnp.dot(row_block, w_gate, preferred_element_type=jnp.float32)
    up_rows = jnp.dot(row_block, w_up, preferred_element_type=jnp.float32)
    hidden = (jax.nn.silu(gate_rows) * up_rows).astype(jnp.bfloat16)
    return jnp.dot(hidden, w_down, preferred_element_type=jnp.float32).astype(jnp.bfloat16)


def relayout(arrived, fs_count, tp_count):
    tile_rows = arrived.shape[2]
    tile_cols = arrived.shape[3]
    grid = arrived.reshape(fs_count, tp_count, tile_rows, tile_cols)
    grid = jnp.transpose(grid, (0, 2, 1, 3))
    return grid.reshape(1, fs_count * tile_rows, tp_count * tile_cols)


def exchange_plan(
    tokens,
    route_ids,
    route_scores,
    norm_gain,
    expert_gate,
    expert_up,
    expert_down,
    shared_gate,
    shared_up,
    shared_down,
):
    fs_count = lax.axis_size("fs")
    tp_count = lax.axis_size("tp")
    experts = fs_count * tp_count
    gain_col = norm_gain[:, None]
    piece_gate = (gain_col[None] * expert_gate).astype(jnp.bfloat16)
    piece_up = (gain_col[None] * expert_up).astype(jnp.bfloat16)
    piece_down = expert_down.astype(jnp.bfloat16)
    moved = (
        lax.all_to_all(piece_gate[:, None], ("fs", "tp"), split_axis=0, concat_axis=1, tiled=True),
        lax.all_to_all(piece_up[:, None], ("fs", "tp"), split_axis=0, concat_axis=1, tiled=True),
        lax.all_to_all(piece_down[:, None], ("fs", "tp"), split_axis=0, concat_axis=1, tiled=True),
    )
    served_gate = relayout(moved[0], fs_count, tp_count)
    served_up = relayout(moved[1], fs_count, tp_count)
    served_down = relayout(moved[2], fs_count, tp_count)
    tile_gate = (gain_col * shared_gate).astype(jnp.bfloat16)
    tile_up = (gain_col * shared_up).astype(jnp.bfloat16)
    tile_down = shared_down.astype(jnp.bfloat16)
    held_gate, held_up, held_down = (
        lax.all_gather(tile_gate, "tp", axis=1, tiled=True),
        lax.all_gather(tile_up, "tp", axis=1, tiled=True),
        lax.all_gather(tile_down, "tp", axis=1, tiled=True),
    )
    rows_dev = tokens.shape[0]
    width = tokens.shape[1]
    picks = route_ids.shape[1]
    capacity = 3 * rows_dev * picks // (2 * experts)
    widened = tokens.astype(jnp.float32)
    normed = (
        widened * lax.rsqrt(jnp.mean(widened * widened, axis=1, keepdims=True) + EPSILON)
    ).astype(jnp.bfloat16)
    weights = route_scale * route_scores / jnp.sum(route_scores, axis=1, keepdims=True)
    flat_ids = route_ids.reshape(-1)
    onehot = (flat_ids[:, None] == jnp.arange(experts, dtype=jnp.int32)[None, :]).astype(jnp.int32)
    earlier = jnp.cumsum(onehot, axis=0) - onehot
    ranks = jnp.sum(earlier * onehot, axis=1)
    target = flat_ids * capacity + ranks
    outbox = (
        jnp.zeros((experts * capacity, width), jnp.bfloat16)
        .at[target]
        .set(jnp.repeat(normed, picks, axis=0))
    )
    arrived = lax.all_to_all(
        outbox.reshape(experts, capacity, width),
        ("fs", "tp"),
        split_axis=0,
        concat_axis=0,
        tiled=True,
    )
    finished = expert_rows(
        arrived.reshape(-1, width), served_gate[0], served_up[0], served_down[0]
    ).reshape(arrived.shape)
    returned = lax.all_to_all(finished, ("fs", "tp"), split_axis=0, concat_axis=0, tiled=True)
    results = returned.reshape(experts * capacity, width)[target]
    routed = jnp.sum(
        results.reshape(rows_dev, picks, width).astype(jnp.float32) * weights[:, :, None], axis=1
    )
    columns = normed
    gate_part = jnp.dot(
        columns,
        lax.all_gather(held_gate, "fs", axis=0, tiled=True),
        preferred_element_type=jnp.float32,
    )
    up_part = jnp.dot(
        columns,
        lax.all_gather(held_up, "fs", axis=0, tiled=True),
        preferred_element_type=jnp.float32,
    )
    shared_hidden = (jax.nn.silu(gate_part) * up_part).astype(jnp.bfloat16)
    columns = shared_hidden
    shared_term = jnp.dot(
        columns,
        lax.all_gather(held_down, "fs", axis=0, tiled=True),
        preferred_element_type=jnp.float32,
    )
    mixed = (routed + shared_term).astype(jnp.bfloat16)
    return (mixed, served_gate, served_up, served_down, held_gate, held_up, held_down)


def silu(value):
    return value / (1.0 + jnp.exp(-value))


def norm_kernel(experts, ids_ref, scores_ref, tokens_ref, out_ref):
    rows, width = tokens_ref.shape
    picks = ids_ref.shape[0]
    extra = out_ref.shape[1] - width
    widened = tokens_ref[...].astype(jnp.float32)
    mean = jnp.mean(widened * widened, axis=1, keepdims=True)
    out_ref[:, :width] = (widened * lax.rsqrt(mean + EPSILON)).astype(jnp.bfloat16)
    scores = scores_ref[...]
    weights = route_scale * scores / jnp.sum(scores, axis=0, keepdims=True)
    place = lax.broadcasted_iota(jnp.int32, (experts, rows), 0)
    dense = jnp.zeros((experts, rows), jnp.float32)
    for k in range(picks):
        dense = dense + jnp.where(ids_ref[k : k + 1, :] == place, weights[k : k + 1, :], 0.0)
    first = dense.astype(jnp.bfloat16).astype(jnp.float32)
    left = dense - first
    second = left.astype(jnp.bfloat16).astype(jnp.float32)
    third = left - second
    blank = jnp.zeros((extra - 3 * experts, rows), jnp.float32)
    stacked = jnp.concatenate([first, second, third, blank], axis=0)
    out_ref[:, width:] = stacked.T.astype(jnp.bfloat16)


def norm_rows(tokens, route_ids, route_scores, experts):
    rows, width = tokens.shape
    extra = ceil_to(3 * experts, LANES)
    return pl.pallas_call(
        functools.partial(norm_kernel, experts),
        out_shape=jax.ShapeDtypeStruct((rows, width + extra), jnp.bfloat16),
        name="norm_rows",
    )(route_ids.T, route_scores.T, tokens)


def pack_kernel(per_step, share, half_ref, gate_ref, up_ref, down_ref, sg_ref, su_ref, sd_ref, gain_ref, out_ref, tail_ref):
    units = gate_ref.shape[1]
    gain = gain_ref[...]
    for j in range(per_step):
        out_ref[j, :units] = (gate_ref[j] * gain).astype(jnp.bfloat16)
        out_ref[j, units : 2 * units] = (up_ref[j] * gain).astype(jnp.bfloat16)
        out_ref[j, 2 * units : 3 * units] = down_ref[j].astype(jnp.bfloat16)
        rows = slice(j * share, (j + 1) * share)
        tail_ref[...] = jnp.zeros(tail_ref.shape, jnp.float32)
        tail_ref[:share] = sg_ref[rows] * gain
        tail_ref[share : 2 * share] = su_ref[rows] * gain
        tail_ref[2 * share : 3 * share] = sd_ref[rows]
        out_ref[j, 3 * units :] = tail_ref[...].astype(jnp.bfloat16)


def pack_tiles(half, halves, gate, up, down, sg, su, sd, gain):
    experts, units, width = gate.shape
    share = sg.shape[0] // experts
    per_step = 8 // math.gcd(share, 8) * 2
    part = width // halves
    tail_rows = ceil_to(3 * share, PACKED_ROWS)
    out_rows = 3 * units + tail_rows
    tile = pl.BlockSpec((per_step, units, part), lambda i, h: (i, 0, h[0]))
    strip = pl.BlockSpec((per_step * share, part), lambda i, h: (i, h[0]))
    return pl.pallas_call(
        functools.partial(pack_kernel, per_step, share),
        grid_spec=pltpu.PrefetchScalarGridSpec(
            num_scalar_prefetch=1,
            grid=(experts // per_step,),
            in_specs=[tile, tile, tile, strip, strip, strip, pl.BlockSpec((1, part), lambda i, h: (0, h[0]))],
            out_specs=pl.BlockSpec((per_step, out_rows, part), lambda i, h: (i, 0, 0)),
            scratch_shapes=[pltpu.VMEM((tail_rows, part), jnp.float32)],
        ),
        out_shape=jax.ShapeDtypeStruct((experts, out_rows, part), jnp.bfloat16),
        name="pack_tiles",
    )(half, gate, up, down, sg, su, sd, gain)


def place_kernel(tp_count, units, halves, half_ref, *refs):
    parts = refs[:halves]
    first_ref, down_ref, shared_ref = refs[halves:]
    part = parts[0].shape[2]
    tail = parts[0].shape[1] - 3 * units
    gate_rows = tp_count * units
    for t in range(tp_count):
        for h in range(halves):
            if halves == 1:
                piece = parts[0][t]
            else:
                piece = jnp.where(half_ref[0] == h, parts[0][t], parts[1][t])
            cols = slice(h * part, (h + 1) * part)
            far = slice((t * halves + h) * part, (t * halves + h + 1) * part)
            first_ref[t * units : (t + 1) * units, cols] = piece[:units]
            first_ref[gate_rows + t * units : gate_rows + (t + 1) * units, cols] = piece[units : 2 * units]
            first_ref[2 * gate_rows + t * tail : 2 * gate_rows + (t + 1) * tail, cols] = piece[3 * units :]
            down_ref[:, far] = piece[2 * units : 3 * units]
            shared_ref[:, far] = piece[3 * units :]
    used = 2 * gate_rows + tp_count * tail
    if used < first_ref.shape[0]:
        first_ref[used:, :] = jnp.zeros((first_ref.shape[0] - used, first_ref.shape[1]), jnp.bfloat16)


def place_tiles(half, parts, fs_count, tp_count, units):
    halves = len(parts)
    rows, part = parts[0].shape[1], parts[0].shape[2]
    tail = rows - 3 * units
    width = halves * part
    first_rows = 2 * tp_count * units + ceil_to(tp_count * tail, LANES)
    block = pl.BlockSpec((tp_count, rows, part), lambda f, h: (f, 0, 0))
    return pl.pallas_call(
        functools.partial(place_kernel, tp_count, units, halves),
        grid_spec=pltpu.PrefetchScalarGridSpec(
            num_scalar_prefetch=1,
            grid=(fs_count,),
            in_specs=[block] * halves,
            out_specs=[
                pl.BlockSpec((first_rows, width), lambda f, h: (0, f)),
                pl.BlockSpec((units, tp_count * width), lambda f, h: (f, 0)),
                pl.BlockSpec((tail, tp_count * width), lambda f, h: (f, 0)),
            ],
        ),
        out_shape=[
            jax.ShapeDtypeStruct((first_rows, fs_count * width), jnp.bfloat16),
            jax.ShapeDtypeStruct((fs_count * units, tp_count * width), jnp.bfloat16),
            jax.ShapeDtypeStruct((fs_count * tail, tp_count * width), jnp.bfloat16),
        ],
        name="place_tiles",
    )(half, *parts)


def ffn_kernel(experts, share, tail, n_keep, own_ref, *refs):
    blocks = refs[: 2 * n_keep]
    first_ref, down_ref, shared_ref, keep_ref, give_ref = refs[2 * n_keep :]
    rows = blocks[0].shape[0]
    hidden_units, width = down_ref.shape
    extra = blocks[0].shape[1] - width
    tokens = jnp.concatenate([b[:, :width] for b in blocks], axis=0)
    marks = jnp.concatenate([b[:, width:] for b in blocks], axis=0).astype(jnp.float32)
    lane = lax.broadcasted_iota(jnp.int32, marks.shape, 1)
    weight = jnp.sum(jnp.where(lax.rem(lane, experts) == own_ref[0], marks, 0.0), axis=1, keepdims=True)
    nt = (((1,), (1,)), ((), ()))
    into = lax.dot_general(tokens, first_ref[...], nt, preferred_element_type=jnp.float32)
    gate = into[:, :hidden_units]
    up = into[:, hidden_units : 2 * hidden_units]
    hidden = (silu(gate) * up).astype(jnp.bfloat16)
    strip = into[:, 2 * hidden_units :]
    lanes = strip.shape[1]
    place = lax.rem(lax.broadcasted_iota(jnp.int32, strip.shape, 1), tail)
    mine = (place >= 2 * share) & (place < 3 * share)
    near = jnp.where(mine, pltpu.roll(strip, 2 * share, 1), 0.0)
    far = jnp.where(mine, pltpu.roll(strip, share, 1), 0.0)
    shared_hidden = (silu(near) * far).astype(jnp.bfloat16)[:, : shared_ref.shape[0]]
    out = weight * jnp.dot(hidden, down_ref[...], preferred_element_type=jnp.float32)
    out = out + jnp.dot(shared_hidden, shared_ref[...], preferred_element_type=jnp.float32)
    out = out.astype(jnp.bfloat16)
    for j in range(n_keep):
        keep_ref[j] = out[j * rows : (j + 1) * rows]
        give_ref[j] = out[(n_keep + j) * rows : (n_keep + j + 1) * rows]


def ffn(own, blocks, first, down, shared, experts, share, tail):
    n_keep = len(blocks) // 2
    rows, width = blocks[0].shape[0], down.shape[1]
    shape = jax.ShapeDtypeStruct((n_keep, rows, width), jnp.bfloat16)
    whole = pl.BlockSpec(memory_space=pltpu.VMEM)
    return pl.pallas_call(
        functools.partial(ffn_kernel, experts, share, tail, n_keep),
        in_specs=[pl.BlockSpec(memory_space=pltpu.SMEM)] + [whole] * (len(blocks) + 3),
        out_specs=[whole, whole],
        out_shape=[shape, shape],
        name="expert_ffn",
    )(own, *blocks, first, down, shared)


def held_kernel(order_ref, *refs):
    tiles = refs[:-4]
    gate_ref, up_ref, down_ref, stage_ref = refs[-4:]
    units = tiles[0].shape[0] // 3
    count = len(tiles)
    width = tiles[0].shape[1]
    for r in range(count):
        spot = pl.multiple_of(order_ref[r] * units, units)
        for m in range(3):
            stage_ref[m, pl.ds(spot, units), :] = tiles[r][m * units : (m + 1) * units, :]
    gate_ref[...] = stage_ref[0].T
    up_ref[...] = stage_ref[1].T
    for t in range(count):
        down_ref[:, t * width : (t + 1) * width] = stage_ref[2, t * units : (t + 1) * units, :]


def held_tiles(order, tiles):
    count = len(tiles)
    units, width = tiles[0].shape[0] // 3, tiles[0].shape[1]
    whole = pl.BlockSpec(memory_space=pltpu.VMEM)
    tall = jax.ShapeDtypeStruct((width, count * units), jnp.bfloat16)
    return pl.pallas_call(
        held_kernel,
        in_specs=[pl.BlockSpec(memory_space=pltpu.SMEM)] + [whole] * count,
        out_specs=[whole] * 3,
        out_shape=[tall, tall, jax.ShapeDtypeStruct((units, count * width), jnp.bfloat16)],
        scratch_shapes=[pltpu.VMEM((3, count * units, width), jnp.bfloat16)],
        name="held_tiles",
    )(order, *tiles)


def gather_plan(
    tokens,
    route_ids,
    route_scores,
    norm_gain,
    expert_gate,
    expert_up,
    expert_down,
    shared_gate,
    shared_up,
    shared_down,
):
    groups = lax.axis_size("grp")
    fs_count = lax.axis_size("fs")
    tp_count = lax.axis_size("tp")
    experts = fs_count * tp_count
    columns = tp_count // CORES
    halves = 2 if groups == 2 else 1
    half = (lax.axis_index("grp") % halves).astype(jnp.int32)[None]
    tp_index = lax.axis_index("tp").astype(jnp.int32)
    own = (lax.axis_index("fs").astype(jnp.int32) * tp_count + tp_index)[None]

    def along_fs(value, k):
        return lax.ppermute(value, "fs", [(i, (i + k) % fs_count) for i in range(fs_count)])

    def along_x(value, j):
        return lax.ppermute(
            value,
            "tp",
            [(i, (i // CORES + j) % columns * CORES + i % CORES) for i in range(tp_count)],
        )

    def across(value):
        return lax.ppermute(value, "tp", [(i, i ^ 1) for i in range(tp_count)])

    gain = norm_gain[None, :]
    gate_t = jnp.transpose(expert_gate, (0, 2, 1))
    up_t = jnp.transpose(expert_up, (0, 2, 1))
    sg_t, su_t = shared_gate.T, shared_up.T
    units = gate_t.shape[1]
    share = sg_t.shape[0] // experts
    packed = pack_tiles(half, halves, gate_t, up_t, expert_down, sg_t, su_t, shared_down, gain)
    tail = packed.shape[1] - 3 * units
    landed = lax.all_to_all(packed, ("fs", "tp"), split_axis=0, concat_axis=0, tiled=True)
    parts = [landed]
    if halves == 2:
        parts.append(lax.ppermute(landed, "grp", [(0, 1), (1, 0)]))

    normed = norm_rows(tokens, route_ids, route_scores, experts)
    chunks = []
    for k in range(fs_count):
        block = normed if k == 0 else along_fs(normed, k)
        column = [block] + [along_x(block, j) for j in range(1, columns)]
        chunks.append(column + [across(b) for b in column])

    first, served_down, shared_rows = place_tiles(half, parts, fs_count, tp_count, units)
    gate_rows = tp_count * units
    served_gate = first[:gate_rows].T
    served_up = first[gate_rows : 2 * gate_rows].T

    sums = []
    for k in range(fs_count):
        keep, give = ffn(own, chunks[k], first, served_down, shared_rows, experts, share, tail)
        got = across(give)
        total = keep[0].astype(jnp.float32) + got[0].astype(jnp.float32)
        for j in range(1, columns):
            step = (keep[j].astype(jnp.float32) + got[j].astype(jnp.float32)).astype(jnp.bfloat16)
            total = total + along_x(step, -j).astype(jnp.float32)
        if k > 0:
            total = along_fs(total.astype(jnp.bfloat16), -k).astype(jnp.float32)
        sums.append(total)
    mixed = sums[0]
    for total in sums[1:]:
        mixed = mixed + total
    mixed = mixed.astype(jnp.bfloat16)

    tile = jnp.concatenate([gain * sg_t, gain * su_t, shared_down], axis=0).astype(jnp.bfloat16)
    tiles, order = [], []
    for j in range(columns):
        tiles.append(tile if j == 0 else along_x(tile, j))
        order.append(((tp_index // CORES - j) % columns) * CORES + tp_index % CORES)
    for j in range(columns):
        tiles.append(across(tiles[j]))
        order.append(order[j] ^ 1)
    held_gate, held_up, held_down = held_tiles(jnp.stack(order), tiles)
    return (mixed, served_gate[None], served_up[None], served_down[None], held_gate, held_up, held_down)


def on_device(tokens, route_ids, *others):
    experts = lax.axis_size("fs") * lax.axis_size("tp")
    if experts <= 2 * route_ids.shape[1]:
        return gather_plan(tokens, route_ids, *others)
    return exchange_plan(tokens, route_ids, *others)


def solution(mesh):
    return jax.shard_map(
        on_device,
        mesh=mesh,
        in_specs=(
            P(("grp", "fs", "tp"), None),
            P(("grp", "fs", "tp"), None),
            P(("grp", "fs", "tp"), None),
            P("fs"),
            P(None, "fs", "tp"),
            P(None, "fs", "tp"),
            P(None, "fs", "tp"),
            P("fs", "tp"),
            P("fs", "tp"),
            P("fs", "tp"),
        ),
        out_specs=(
            P(("grp", "fs", "tp"), None),
            P(("grp", "fs", "tp"), None, None),
            P(("grp", "fs", "tp"), None, None),
            P(("grp", "fs", "tp"), None, None),
            P(("grp", "fs"), None),
            P(("grp", "fs"), None),
            P(("grp", "fs"), None),
        ),
        check_vma=False,
    )
```

```python
import functools

import jax
import jax.numpy as jnp
from jax import lax
from jax.experimental import pallas as pl
from jax.experimental.pallas import tpu as pltpu
from jax.sharding import PartitionSpec as P


EPSILON = 1e-06
route_scale = 2.5
LANES = 128
PACKED_ROWS = 16
CORES = 2
IN_VMEM = pl.BlockSpec(memory_space=pltpu.VMEM)
IN_SMEM = pl.BlockSpec(memory_space=pltpu.SMEM)
SMALL_GRANT = pltpu.CompilerParams(vmem_limit_bytes=16 * 1024 * 1024)


def ceil_to(value, unit):
    return -(-value // unit) * unit


def expert_rows(row_block, w_gate, w_up, w_down):
    gate_rows = jnp.dot(row_block, w_gate, preferred_element_type=jnp.float32)
    up_rows = jnp.dot(row_block, w_up, preferred_element_type=jnp.float32)
    hidden = (jax.nn.silu(gate_rows) * up_rows).astype(jnp.bfloat16)
    return jnp.dot(hidden, w_down, preferred_element_type=jnp.float32).astype(jnp.bfloat16)


def relayout(arrived, fs_count, tp_count):
    tile_rows = arrived.shape[2]
    tile_cols = arrived.shape[3]
    grid = arrived.reshape(fs_count, tp_count, tile_rows, tile_cols)
    grid = jnp.transpose(grid, (0, 2, 1, 3))
    return grid.reshape(1, fs_count * tile_rows, tp_count * tile_cols)


def exchange_plan(
    tokens,
    route_ids,
    route_scores,
    norm_gain,
    expert_gate,
    expert_up,
    expert_down,
    shared_gate,
    shared_up,
    shared_down,
):
    fs_count = lax.axis_size("fs")
    tp_count = lax.axis_size("tp")
    experts = fs_count * tp_count
    gain_col = norm_gain[:, None]
    piece_gate = (gain_col[None] * expert_gate).astype(jnp.bfloat16)
    piece_up = (gain_col[None] * expert_up).astype(jnp.bfloat16)
    piece_down = expert_down.astype(jnp.bfloat16)
    moved = (
        lax.all_to_all(piece_gate[:, None], ("fs", "tp"), split_axis=0, concat_axis=1, tiled=True),
        lax.all_to_all(piece_up[:, None], ("fs", "tp"), split_axis=0, concat_axis=1, tiled=True),
        lax.all_to_all(piece_down[:, None], ("fs", "tp"), split_axis=0, concat_axis=1, tiled=True),
    )
    served_gate = relayout(moved[0], fs_count, tp_count)
    served_up = relayout(moved[1], fs_count, tp_count)
    served_down = relayout(moved[2], fs_count, tp_count)
    tile_gate = (gain_col * shared_gate).astype(jnp.bfloat16)
    tile_up = (gain_col * shared_up).astype(jnp.bfloat16)
    tile_down = shared_down.astype(jnp.bfloat16)
    held_gate, held_up, held_down = (
        lax.all_gather(tile_gate, "tp", axis=1, tiled=True),
        lax.all_gather(tile_up, "tp", axis=1, tiled=True),
        lax.all_gather(tile_down, "tp", axis=1, tiled=True),
    )
    rows_dev = tokens.shape[0]
    width = tokens.shape[1]
    picks = route_ids.shape[1]
    capacity = 3 * rows_dev * picks // (2 * experts)
    widened = tokens.astype(jnp.float32)
    normed = (
        widened * lax.rsqrt(jnp.mean(widened * widened, axis=1, keepdims=True) + EPSILON)
    ).astype(jnp.bfloat16)
    weights = route_scale * route_scores / jnp.sum(route_scores, axis=1, keepdims=True)
    flat_ids = route_ids.reshape(-1)
    onehot = (flat_ids[:, None] == jnp.arange(experts, dtype=jnp.int32)[None, :]).astype(jnp.int32)
    earlier = jnp.cumsum(onehot, axis=0) - onehot
    ranks = jnp.sum(earlier * onehot, axis=1)
    target = flat_ids * capacity + ranks
    outbox = (
        jnp.zeros((experts * capacity, width), jnp.bfloat16)
        .at[target]
        .set(jnp.repeat(normed, picks, axis=0))
    )
    arrived = lax.all_to_all(
        outbox.reshape(experts, capacity, width),
        ("fs", "tp"),
        split_axis=0,
        concat_axis=0,
        tiled=True,
    )
    finished = expert_rows(
        arrived.reshape(-1, width), served_gate[0], served_up[0], served_down[0]
    ).reshape(arrived.shape)
    returned = lax.all_to_all(finished, ("fs", "tp"), split_axis=0, concat_axis=0, tiled=True)
    results = returned.reshape(experts * capacity, width)[target]
    routed = jnp.sum(
        results.reshape(rows_dev, picks, width).astype(jnp.float32) * weights[:, :, None], axis=1
    )
    columns = normed
    gate_part = jnp.dot(
        columns,
        lax.all_gather(held_gate, "fs", axis=0, tiled=True),
        preferred_element_type=jnp.float32,
    )
    up_part = jnp.dot(
        columns,
        lax.all_gather(held_up, "fs", axis=0, tiled=True),
        preferred_element_type=jnp.float32,
    )
    shared_hidden = (jax.nn.silu(gate_part) * up_part).astype(jnp.bfloat16)
    columns = shared_hidden
    shared_term = jnp.dot(
        columns,
        lax.all_gather(held_down, "fs", axis=0, tiled=True),
        preferred_element_type=jnp.float32,
    )
    mixed = (routed + shared_term).astype(jnp.bfloat16)
    return (mixed, served_gate, served_up, served_down, held_gate, held_up, held_down)


def silu(value):
    return value / (1.0 + jnp.exp(-value))


def norm_kernel(experts, tiles, half_ref, ids_ref, scores_ref, tokens_ref, low_ref, high_ref):
    rows, width = tokens_ref.shape
    picks = ids_ref.shape[0]
    extra = low_ref.shape[1] - width
    widened = tokens_ref[...].astype(jnp.float32)
    mean = jnp.mean(widened * widened, axis=1, keepdims=True)
    normed = (widened * lax.rsqrt(mean + EPSILON)).astype(jnp.bfloat16)
    scores = scores_ref[...]
    weights = route_scale * scores / jnp.sum(scores, axis=0, keepdims=True)
    place = lax.broadcasted_iota(jnp.int32, (experts, rows), 0)
    dense = jnp.zeros((experts, rows), jnp.float32)
    for k in range(picks):
        dense = dense + jnp.where(ids_ref[k : k + 1, :] == place, weights[k : k + 1, :], 0.0)
    first = dense.astype(jnp.bfloat16).astype(jnp.float32)
    left = dense - first
    second = left.astype(jnp.bfloat16).astype(jnp.float32)
    third = left - second
    blank = jnp.zeros((extra - 3 * experts, rows), jnp.float32)
    marks = jnp.concatenate([first, second, third, blank], axis=0).T.astype(jnp.bfloat16)
    part = width // tiles // 2
    swap = half_ref[0] != 0
    for n, ref in enumerate((low_ref, high_ref)):
        mine = slice(n * (rows // 2), (n + 1) * (rows // 2))
        for i in range(tiles):
            left_cols = normed[mine, (2 * i) * part : (2 * i + 1) * part]
            right_cols = normed[mine, (2 * i + 1) * part : (2 * i + 2) * part]
            ref[:, i * part : (i + 1) * part] = jnp.where(swap, right_cols, left_cols)
            far = slice(width // 2 + i * part, width // 2 + (i + 1) * part)
            ref[:, far] = jnp.where(swap, left_cols, right_cols)
        ref[:, width:] = marks[mine]


def norm_rows(half, tokens, route_ids, route_scores, experts, tiles):
    rows, width = tokens.shape
    extra = ceil_to(3 * experts, LANES)
    shape = jax.ShapeDtypeStruct((rows // 2, width + extra), jnp.bfloat16)
    return pl.pallas_call(
        functools.partial(norm_kernel, experts, tiles),
        in_specs=[IN_SMEM] + [IN_VMEM] * 3,
        out_specs=[IN_VMEM] * 2,
        out_shape=[shape, shape],
        compiler_params=SMALL_GRANT,
        name="norm_rows",
    )(half, route_ids.T, route_scores.T, tokens)


def pack_kernel(per_step, share, half_ref, gate_ref, up_ref, down_ref, sg_ref, su_ref, sd_ref, gain_ref, out_ref, tail_ref):
    units = gate_ref.shape[1]
    gain = gain_ref[...]
    for j in range(per_step):
        out_ref[j, :units] = (gate_ref[j] * gain).astype(jnp.bfloat16)
        out_ref[j, units : 2 * units] = (up_ref[j] * gain).astype(jnp.bfloat16)
        out_ref[j, 2 * units : 3 * units] = down_ref[j].astype(jnp.bfloat16)
        rows = slice(j * share, (j + 1) * share)
        tail_ref[...] = jnp.zeros(tail_ref.shape, jnp.float32)
        tail_ref[:share] = sg_ref[rows] * gain
        tail_ref[share : 2 * share] = su_ref[rows] * gain
        tail_ref[2 * share : 3 * share] = sd_ref[rows]
        out_ref[j, 3 * units :] = tail_ref[...].astype(jnp.bfloat16)


def pack_tiles(half, gate, up, down, sg, su, sd, gain):
    experts, units, width = gate.shape
    share = sg.shape[0] // experts
    per_step = experts // 4
    part = width // 2
    tail_rows = ceil_to(3 * share, PACKED_ROWS)
    out_rows = 3 * units + tail_rows
    tile = pl.BlockSpec((per_step, units, part), lambda i, h: (i, 0, h[0]))
    strip = pl.BlockSpec((per_step * share, part), lambda i, h: (i, h[0]))
    return pl.pallas_call(
        functools.partial(pack_kernel, per_step, share),
        grid_spec=pltpu.PrefetchScalarGridSpec(
            num_scalar_prefetch=1,
            grid=(experts // per_step,),
            in_specs=[tile, tile, tile, strip, strip, strip, pl.BlockSpec((1, part), lambda i, h: (0, h[0]))],
            out_specs=pl.BlockSpec((per_step, out_rows, part), lambda i, h: (i, 0, 0)),
            scratch_shapes=[pltpu.VMEM((tail_rows, part), jnp.float32)],
        ),
        out_shape=jax.ShapeDtypeStruct((experts, out_rows, part), jnp.bfloat16),
        compiler_params=SMALL_GRANT,
        name="pack_tiles",
    )(half, gate, up, down, sg, su, sd, gain)


def place_kernel(fs_count, tp_count, units, in_ref, out_ref):
    part = in_ref.shape[2]
    tail = in_ref.shape[1] - 3 * units
    gate_rows = tp_count * units
    strip_at = 2 * gate_rows
    down_at = strip_at + tp_count * tail
    shared_at = down_at + fs_count * units
    for f in range(fs_count):
        for t in range(tp_count):
            src = f * tp_count + t
            cols = slice(f * part, (f + 1) * part)
            out_ref[t * units : (t + 1) * units, cols] = in_ref[src, :units]
            out_ref[gate_rows + t * units : gate_rows + (t + 1) * units, cols] = in_ref[src, units : 2 * units]
            last = in_ref[src, 3 * units :]
            out_ref[strip_at + t * tail : strip_at + (t + 1) * tail, cols] = last
            cols = slice(t * part, (t + 1) * part)
            out_ref[down_at + f * units : down_at + (f + 1) * units, cols] = in_ref[src, 2 * units : 3 * units]
            out_ref[shared_at + f * tail : shared_at + (f + 1) * tail, cols] = last


def place_tiles(landed, fs_count, tp_count, units):
    rows, part = landed.shape[1:]
    tail = rows - 3 * units
    out_rows = 2 * tp_count * units + tp_count * tail + fs_count * (units + tail)
    return pl.pallas_call(
        functools.partial(place_kernel, fs_count, tp_count, units),
        in_specs=[IN_VMEM],
        out_specs=IN_VMEM,
        out_shape=jax.ShapeDtypeStruct((out_rows, fs_count * part), jnp.bfloat16),
        compiler_params=SMALL_GRANT,
        name="place_tiles",
    )(landed)


def ffn_kernel(experts, gate_rows, strip_rows, down_rows, share, tail, count, own_ref, *refs):
    blocks = refs[:count]
    own_low, peer_low, own_high, peer_high = refs[count : count + 4]
    outs = refs[count + 4 :]
    rows, part = blocks[0].shape[0], own_low.shape[1]
    width = 2 * part
    low = jnp.concatenate([b[:, :part] for b in blocks], axis=0)
    high = jnp.concatenate([b[:, part:width] for b in blocks], axis=0)
    marks = jnp.concatenate([b[:, width:] for b in blocks], axis=0).astype(jnp.float32)
    lane = lax.rem(lax.broadcasted_iota(jnp.int32, marks.shape, 1), experts)
    strip_at = 2 * gate_rows
    down_at = strip_at + strip_rows
    shared_at = down_at + down_rows

    def into(a, b):
        nt = (((1,), (1,)), ((), ()))
        return lax.dot_general(a, b, nt, preferred_element_type=jnp.float32)

    def onto(a, b):
        return jnp.dot(a, b, preferred_element_type=jnp.float32)

    hidden = []
    for n, (near, far) in enumerate(((own_low, own_high), (peer_low, peer_high))):
        weight = jnp.sum(jnp.where(lane == own_ref[n], marks, 0.0), axis=1, keepdims=True)
        both = into(low, near[:strip_at]) + into(high, far[:strip_at])
        hidden.append((weight * silu(both[:, :gate_rows]) * both[:, gate_rows:]).astype(jnp.bfloat16))
    near = jnp.concatenate([own_low[strip_at:down_at], peer_low[strip_at:down_at]], axis=0)
    far = jnp.concatenate([own_high[strip_at:down_at], peer_high[strip_at:down_at]], axis=0)
    strip = into(low, near) + into(high, far)
    place = lax.rem(lax.broadcasted_iota(jnp.int32, strip.shape, 1), tail)
    mine = (place >= 2 * share) & (place < 3 * share)
    gate = jnp.where(mine, pltpu.roll(strip, 2 * share, 1), 0.0)
    up = jnp.where(mine, pltpu.roll(strip, share, 1), 0.0)
    shared_hidden = (silu(gate) * up).astype(jnp.bfloat16)
    for n, (own, peer) in enumerate(((own_low, peer_low), (own_high, peer_high))):
        shared = jnp.concatenate([own[shared_at:], peer[shared_at:]], axis=0)
        total = onto(hidden[0], own[down_at:shared_at]) + onto(hidden[1], peer[down_at:shared_at])
        total = (total + onto(shared_hidden, shared)).astype(jnp.bfloat16)
        for j in range(count):
            outs[j][:, n * part : (n + 1) * part] = total[j * rows : (j + 1) * rows]


def ffn(own, blocks, mats, experts, sizes):
    rows, width = blocks[0].shape[0], 2 * mats[0].shape[1]
    shape = jax.ShapeDtypeStruct((rows, width), jnp.bfloat16)
    return pl.pallas_call(
        functools.partial(ffn_kernel, experts, *sizes, len(blocks)),
        in_specs=[IN_SMEM] + [IN_VMEM] * (len(blocks) + 4),
        out_specs=[IN_VMEM] * len(blocks),
        out_shape=[shape] * len(blocks),
        compiler_params=SMALL_GRANT,
        name="expert_ffn",
    )(own, *blocks, *mats)


def finish_kernel(tiles, half_ref, *refs):
    out_ref = refs[-1]
    rows, width = out_ref.shape
    part = width // tiles // 2
    swap = half_ref[0] != 0
    for n in range(2):
        mine = slice(n * (rows // 2), (n + 1) * (rows // 2))
        terms = refs[3 * n : 3 * n + 3]
        total = terms[0][...].astype(jnp.float32) + terms[1][...].astype(jnp.float32)
        total = (total + terms[2][...].astype(jnp.float32)).astype(jnp.bfloat16)
        for i in range(tiles):
            near = total[:, i * part : (i + 1) * part]
            far = total[:, width // 2 + i * part : width // 2 + (i + 1) * part]
            out_ref[mine, (2 * i) * part : (2 * i + 1) * part] = jnp.where(swap, far, near)
            out_ref[mine, (2 * i + 1) * part : (2 * i + 2) * part] = jnp.where(swap, near, far)


def finish(half, terms, tiles):
    rows, width = terms[0].shape
    return pl.pallas_call(
        functools.partial(finish_kernel, tiles),
        in_specs=[IN_SMEM] + [IN_VMEM] * len(terms),
        out_specs=IN_VMEM,
        out_shape=jax.ShapeDtypeStruct((2 * rows, width), jnp.bfloat16),
        compiler_params=SMALL_GRANT,
        name="finish",
    )(half, *terms)


def serve_kernel(fs_count, tp_count, gate_rows, down_at, half_ref, low_ref, high_ref, gate_ref, up_ref, down_ref):
    part = low_ref.shape[1] // fs_count
    swap = half_ref[0] != 0
    for f in range(fs_count):
        cols = slice(f * part, (f + 1) * part)
        for n, ref in enumerate((gate_ref, up_ref)):
            rows = slice(n * gate_rows, (n + 1) * gate_rows)
            near, far = low_ref[rows, cols], high_ref[rows, cols]
            ref[(2 * f) * part : (2 * f + 1) * part, :] = jnp.where(swap, far, near).T
            ref[(2 * f + 1) * part : (2 * f + 2) * part, :] = jnp.where(swap, near, far).T
    rows = slice(down_at, down_at + down_ref.shape[0])
    part = low_ref.shape[1] // tp_count
    for t in range(tp_count):
        cols = slice(t * part, (t + 1) * part)
        near, far = low_ref[rows, cols], high_ref[rows, cols]
        down_ref[:, (2 * t) * part : (2 * t + 1) * part] = jnp.where(swap, far, near)
        down_ref[:, (2 * t + 1) * part : (2 * t + 2) * part] = jnp.where(swap, near, far)


def serve(half, low, high, fs_count, tp_count, gate_rows, down_at, down_rows):
    width = 2 * low.shape[1]
    tall = jax.ShapeDtypeStruct((width, gate_rows), jnp.bfloat16)
    return pl.pallas_call(
        functools.partial(serve_kernel, fs_count, tp_count, gate_rows, down_at),
        in_specs=[IN_SMEM, IN_VMEM, IN_VMEM],
        out_specs=[IN_VMEM] * 3,
        out_shape=[tall, tall, jax.ShapeDtypeStruct((down_rows, width), jnp.bfloat16)],
        compiler_params=SMALL_GRANT,
        name="serve",
    )(half, low, high)


def held_kernel(order_ref, *refs):
    tiles = refs[:-4]
    gate_ref, up_ref, down_ref, stage_ref = refs[-4:]
    units = tiles[0].shape[0] // 3
    count = len(tiles)
    width = tiles[0].shape[1]
    for r in range(count):
        spot = pl.multiple_of(order_ref[r] * units, units)
        for m in range(3):
            stage_ref[m, pl.ds(spot, units), :] = tiles[r][m * units : (m + 1) * units, :]
    gate_ref[...] = stage_ref[0].T
    up_ref[...] = stage_ref[1].T
    for t in range(count):
        down_ref[:, t * width : (t + 1) * width] = stage_ref[2, t * units : (t + 1) * units, :]


def held_tiles(order, tiles):
    count = len(tiles)
    units, width = tiles[0].shape[0] // 3, tiles[0].shape[1]
    tall = jax.ShapeDtypeStruct((width, count * units), jnp.bfloat16)
    return pl.pallas_call(
        held_kernel,
        in_specs=[IN_SMEM] + [IN_VMEM] * count,
        out_specs=[IN_VMEM] * 3,
        out_shape=[tall, tall, jax.ShapeDtypeStruct((units, count * width), jnp.bfloat16)],
        scratch_shapes=[pltpu.VMEM((3, count * units, width), jnp.bfloat16)],
        compiler_params=SMALL_GRANT,
        name="held_tiles",
    )(order, *tiles)


OUT_STREAMS = (("pa", 1, 0), ("nb", -1, 1), ("pb", 1, 1), ("na", -1, 0))


def gather_plan(
    tokens,
    route_ids,
    route_scores,
    norm_gain,
    expert_gate,
    expert_up,
    expert_down,
    shared_gate,
    shared_up,
    shared_down,
):
    fs_count = lax.axis_size("fs")
    tp_count = lax.axis_size("tp")
    experts = fs_count * tp_count
    ring = 2 * fs_count
    hops = fs_count
    half = lax.axis_index("grp").astype(jnp.int32)[None]
    tp_index = lax.axis_index("tp").astype(jnp.int32)
    me = lax.axis_index("fs").astype(jnp.int32) * tp_count + tp_index
    own = jnp.stack([me, me ^ 1])

    def spot(position, core):
        position = position % ring
        if position < fs_count:
            return position * tp_count + core
        return (ring - 1 - position) * tp_count + CORES + core

    def around(value, way):
        moves = [(spot(p, c), spot(p + way, c)) for p in range(ring) for c in range(CORES)]
        return lax.ppermute(value, ("fs", "tp"), moves)

    def across(value):
        return lax.ppermute(value, "tp", [(i, i ^ 1) for i in range(tp_count)])

    def sideways(value):
        return lax.ppermute(value, "tp", [(i, i ^ CORES) for i in range(tp_count)])

    gain = norm_gain[None, :]
    gate_t = jnp.transpose(expert_gate, (0, 2, 1))
    up_t = jnp.transpose(expert_up, (0, 2, 1))
    sg_t, su_t = shared_gate.T, shared_up.T
    units = gate_t.shape[1]
    share = sg_t.shape[0] // experts
    packed = pack_tiles(half, gate_t, up_t, expert_down, sg_t, su_t, shared_down, gain)
    tail = packed.shape[1] - 3 * units
    gate_rows, strip_rows = tp_count * units, tp_count * tail
    down_rows = fs_count * units
    down_at = 2 * gate_rows + strip_rows
    landed = lax.all_to_all(packed, ("fs", "tp"), split_axis=0, concat_axis=0, tiled=True)
    own_low = place_tiles(landed, fs_count, tp_count, units)
    own_high = lax.ppermute(own_low, "grp", [(0, 1), (1, 0)])
    peer_low = across(own_low)
    peer_high = across(own_high)
    mats = (own_low, peer_low, own_high, peer_high)

    seen = {}
    pair = norm_rows(half, tokens, route_ids, route_scores, experts, fs_count)
    for name, _, n in OUT_STREAMS:
        seen[name] = [pair[n]]
    for s in range(1, hops + 1):
        for name, way, _ in OUT_STREAMS:
            if s < hops or name in ("pa", "nb"):
                seen[name].append(around(seen[name][-1], way))

    sizes = (gate_rows, strip_rows, down_rows, share, tail)
    made = {name: {} for name in seen}
    for s in range(hops, 0, -1):
        keys = [(name, s) for name, _, _ in OUT_STREAMS if s < len(seen[name])]
        if s == 1:
            keys += [("pa", 0), ("pb", 0)]
        outs = ffn(own, [seen[name][d] for name, d in keys], mats, experts, sizes)
        for (name, d), out in zip(keys, outs):
            made[name][d] = out

    ended = {}
    for name, way, _ in OUT_STREAMS:
        deepest = max(made[name])
        moving = made[name][deepest]
        for d in range(deepest - 1, -1, -1):
            moving = around(moving, -way)
            if d > 0:
                moving = (moving.astype(jnp.float32) + made[name][d].astype(jnp.float32)).astype(jnp.bfloat16)
        ended[name] = moving
    terms = (made["pa"][0], ended["pa"], ended["na"], made["pb"][0], ended["pb"], ended["nb"])
    mixed = finish(half, terms, tp_count)

    served_gate, served_up, served_down = serve(
        half, own_low, own_high, fs_count, tp_count, gate_rows, down_at, down_rows
    )

    tile = jnp.concatenate([gain * sg_t, gain * su_t, shared_down], axis=0).astype(jnp.bfloat16)
    tiles = [tile, sideways(tile)]
    tiles += [across(tiles[0]), across(tiles[1])]
    order = jnp.stack([tp_index, tp_index ^ CORES, tp_index ^ 1, tp_index ^ (CORES + 1)])
    held_gate, held_up, held_down = held_tiles(order, tiles)
    return (mixed, served_gate[None], served_up[None], served_down[None], held_gate, held_up, held_down)


def gathers(experts, picks, groups, columns):
    return experts <= 2 * picks and groups == 2 and columns == 2 * CORES


def on_device(tokens, route_ids, *others):
    fs_count, tp_count = lax.axis_size("fs"), lax.axis_size("tp")
    if gathers(fs_count * tp_count, route_ids.shape[1], lax.axis_size("grp"), tp_count):
        return gather_plan(tokens, route_ids, *others)
    return exchange_plan(tokens, route_ids, *others)


def solution(mesh):
    return jax.shard_map(
        on_device,
        mesh=mesh,
        in_specs=(
            P(("grp", "fs", "tp"), None),
            P(("grp", "fs", "tp"), None),
            P(("grp", "fs", "tp"), None),
            P("fs"),
            P(None, "fs", "tp"),
            P(None, "fs", "tp"),
            P(None, "fs", "tp"),
            P("fs", "tp"),
            P("fs", "tp"),
            P("fs", "tp"),
        ),
        out_specs=(
            P(("grp", "fs", "tp"), None),
            P(("grp", "fs", "tp"), None, None),
            P(("grp", "fs", "tp"), None, None),
            P(("grp", "fs", "tp"), None, None),
            P(("grp", "fs"), None),
            P(("grp", "fs"), None),
            P(("grp", "fs"), None),
        ),
        check_vma=False,
    )
```

```python
import functools

import jax
import jax.numpy as jnp
from jax import lax
from jax.experimental import pallas as pl
from jax.experimental.pallas import tpu as pltpu
from jax.sharding import PartitionSpec as P


EPSILON = 1e-06
route_scale = 2.5
LANES = 128
PACKED_ROWS = 16
CORES = 2
IN_VMEM = pl.BlockSpec(memory_space=pltpu.VMEM)
IN_SMEM = pl.BlockSpec(memory_space=pltpu.SMEM)
SMALL_GRANT = pltpu.CompilerParams(vmem_limit_bytes=16 * 1024 * 1024)


def ceil_to(value, unit):
    return -(-value // unit) * unit


def expert_rows(row_block, w_gate, w_up, w_down):
    gate_rows = jnp.dot(row_block, w_gate, preferred_element_type=jnp.float32)
    up_rows = jnp.dot(row_block, w_up, preferred_element_type=jnp.float32)
    hidden = (jax.nn.silu(gate_rows) * up_rows).astype(jnp.bfloat16)
    return jnp.dot(hidden, w_down, preferred_element_type=jnp.float32).astype(jnp.bfloat16)


def relayout(arrived, fs_count, tp_count):
    tile_rows = arrived.shape[2]
    tile_cols = arrived.shape[3]
    grid = arrived.reshape(fs_count, tp_count, tile_rows, tile_cols)
    grid = jnp.transpose(grid, (0, 2, 1, 3))
    return grid.reshape(1, fs_count * tile_rows, tp_count * tile_cols)


def exchange_plan(
    tokens,
    route_ids,
    route_scores,
    norm_gain,
    expert_gate,
    expert_up,
    expert_down,
    shared_gate,
    shared_up,
    shared_down,
):
    fs_count = lax.axis_size("fs")
    tp_count = lax.axis_size("tp")
    experts = fs_count * tp_count
    gain_col = norm_gain[:, None]
    piece_gate = (gain_col[None] * expert_gate).astype(jnp.bfloat16)
    piece_up = (gain_col[None] * expert_up).astype(jnp.bfloat16)
    piece_down = expert_down.astype(jnp.bfloat16)
    moved = (
        lax.all_to_all(piece_gate[:, None], ("fs", "tp"), split_axis=0, concat_axis=1, tiled=True),
        lax.all_to_all(piece_up[:, None], ("fs", "tp"), split_axis=0, concat_axis=1, tiled=True),
        lax.all_to_all(piece_down[:, None], ("fs", "tp"), split_axis=0, concat_axis=1, tiled=True),
    )
    served_gate = relayout(moved[0], fs_count, tp_count)
    served_up = relayout(moved[1], fs_count, tp_count)
    served_down = relayout(moved[2], fs_count, tp_count)
    tile_gate = (gain_col * shared_gate).astype(jnp.bfloat16)
    tile_up = (gain_col * shared_up).astype(jnp.bfloat16)
    tile_down = shared_down.astype(jnp.bfloat16)
    held_gate, held_up, held_down = (
        lax.all_gather(tile_gate, "tp", axis=1, tiled=True),
        lax.all_gather(tile_up, "tp", axis=1, tiled=True),
        lax.all_gather(tile_down, "tp", axis=1, tiled=True),
    )
    rows_dev = tokens.shape[0]
    width = tokens.shape[1]
    picks = route_ids.shape[1]
    capacity = 3 * rows_dev * picks // (2 * experts)
    widened = tokens.astype(jnp.float32)
    normed = (
        widened * lax.rsqrt(jnp.mean(widened * widened, axis=1, keepdims=True) + EPSILON)
    ).astype(jnp.bfloat16)
    weights = route_scale * route_scores / jnp.sum(route_scores, axis=1, keepdims=True)
    flat_ids = route_ids.reshape(-1)
    onehot = (flat_ids[:, None] == jnp.arange(experts, dtype=jnp.int32)[None, :]).astype(jnp.int32)
    earlier = jnp.cumsum(onehot, axis=0) - onehot
    ranks = jnp.sum(earlier * onehot, axis=1)
    target = flat_ids * capacity + ranks
    outbox = (
        jnp.zeros((experts * capacity, width), jnp.bfloat16)
        .at[target]
        .set(jnp.repeat(normed, picks, axis=0))
    )
    arrived = lax.all_to_all(
        outbox.reshape(experts, capacity, width),
        ("fs", "tp"),
        split_axis=0,
        concat_axis=0,
        tiled=True,
    )
    finished = expert_rows(
        arrived.reshape(-1, width), served_gate[0], served_up[0], served_down[0]
    ).reshape(arrived.shape)
    returned = lax.all_to_all(finished, ("fs", "tp"), split_axis=0, concat_axis=0, tiled=True)
    results = returned.reshape(experts * capacity, width)[target]
    routed = jnp.sum(
        results.reshape(rows_dev, picks, width).astype(jnp.float32) * weights[:, :, None], axis=1
    )
    columns = normed
    gate_part = jnp.dot(
        columns,
        lax.all_gather(held_gate, "fs", axis=0, tiled=True),
        preferred_element_type=jnp.float32,
    )
    up_part = jnp.dot(
        columns,
        lax.all_gather(held_up, "fs", axis=0, tiled=True),
        preferred_element_type=jnp.float32,
    )
    shared_hidden = (jax.nn.silu(gate_part) * up_part).astype(jnp.bfloat16)
    columns = shared_hidden
    shared_term = jnp.dot(
        columns,
        lax.all_gather(held_down, "fs", axis=0, tiled=True),
        preferred_element_type=jnp.float32,
    )
    mixed = (routed + shared_term).astype(jnp.bfloat16)
    return (mixed, served_gate, served_up, served_down, held_gate, held_up, held_down)


def silu(value):
    return value / (1.0 + jnp.exp(-value))


def norm_kernel(experts, tiles, half_ref, ids_ref, scores_ref, tokens_ref, low_ref, high_ref):
    rows, width = tokens_ref.shape
    picks = ids_ref.shape[0]
    span = (low_ref.shape[1] - width) // 2
    widened = tokens_ref[...].astype(jnp.float32)
    mean = jnp.mean(widened * widened, axis=1, keepdims=True)
    normed = (widened * lax.rsqrt(mean + EPSILON)).astype(jnp.bfloat16)
    scores = scores_ref[...]
    weights = route_scale * scores / jnp.sum(scores, axis=0, keepdims=True)
    place = lax.broadcasted_iota(jnp.int32, (experts, rows), 0)
    dense = jnp.zeros((experts, rows), jnp.float32)
    for k in range(picks):
        dense = dense + jnp.where(ids_ref[k : k + 1, :] == place, weights[k : k + 1, :], 0.0)
    first = dense.astype(jnp.bfloat16).astype(jnp.float32)
    left = dense - first
    second = left.astype(jnp.bfloat16).astype(jnp.float32)
    third = left - second
    blank = jnp.zeros((span - 3 * experts, rows), jnp.float32)
    stacked = jnp.concatenate([first, second, third, blank], axis=0)
    marks = jnp.concatenate([stacked, stacked], axis=0).T.astype(jnp.bfloat16)
    low_ref[:, width : width + span] = marks[: rows // 2, :span]
    low_ref[:, width + span :] = marks[rows // 2 :, span:]
    part = width // tiles // 2
    swap = half_ref[0] != 0
    for n, ref in enumerate((low_ref, high_ref)):
        mine = slice(n * (rows // 2), (n + 1) * (rows // 2))
        for i in range(tiles):
            left_cols = normed[mine, (2 * i) * part : (2 * i + 1) * part]
            right_cols = normed[mine, (2 * i + 1) * part : (2 * i + 2) * part]
            ref[:, i * part : (i + 1) * part] = jnp.where(swap, right_cols, left_cols)
            far = slice(width // 2 + i * part, width // 2 + (i + 1) * part)
            ref[:, far] = jnp.where(swap, left_cols, right_cols)


def norm_rows(half, tokens, route_ids, route_scores, experts, tiles):
    rows, width = tokens.shape
    extra = 2 * ceil_to(3 * experts, LANES // 2)
    return pl.pallas_call(
        functools.partial(norm_kernel, experts, tiles),
        in_specs=[IN_SMEM] + [IN_VMEM] * 3,
        out_specs=[IN_VMEM] * 2,
        out_shape=[
            jax.ShapeDtypeStruct((rows // 2, width + extra), jnp.bfloat16),
            jax.ShapeDtypeStruct((rows // 2, width), jnp.bfloat16),
        ],
        compiler_params=SMALL_GRANT,
        name="norm_rows",
    )(half, route_ids.T, route_scores.T, tokens)


def pack_in_kernel(half_ref, gate_ref, up_ref, gain_ref, out_ref):
    units = gate_ref.shape[1]
    gain = gain_ref[...]
    for j in range(gate_ref.shape[0]):
        out_ref[j, :units] = (gate_ref[j] * gain).astype(jnp.bfloat16)
        out_ref[j, units:] = (up_ref[j] * gain).astype(jnp.bfloat16)


def pack_in(half, gate, up, gain):
    experts, units, width = gate.shape
    per_step = experts // 2
    part = width // 2
    tile = pl.BlockSpec((per_step, units, part), lambda i, h: (i, 0, h[0]))
    return pl.pallas_call(
        pack_in_kernel,
        grid_spec=pltpu.PrefetchScalarGridSpec(
            num_scalar_prefetch=1,
            grid=(experts // per_step,),
            in_specs=[tile, tile, pl.BlockSpec((1, part), lambda i, h: (0, h[0]))],
            out_specs=pl.BlockSpec((per_step, 2 * units, part), lambda i, h: (i, 0, 0)),
        ),
        out_shape=jax.ShapeDtypeStruct((experts, 2 * units, part), jnp.bfloat16),
        name="pack_in",
    )(half, gate, up, gain)


def pack_out_kernel(share, half_ref, down_ref, sg_ref, su_ref, sd_ref, gain_ref, out_ref, tail_ref):
    units = down_ref.shape[1]
    gain = gain_ref[...]
    for j in range(down_ref.shape[0]):
        out_ref[j, :units] = down_ref[j].astype(jnp.bfloat16)
        rows = slice(j * share, (j + 1) * share)
        tail_ref[...] = jnp.zeros(tail_ref.shape, jnp.float32)
        tail_ref[:share] = sg_ref[rows] * gain
        tail_ref[share : 2 * share] = su_ref[rows] * gain
        tail_ref[2 * share : 3 * share] = sd_ref[rows]
        out_ref[j, units:] = tail_ref[...].astype(jnp.bfloat16)


def pack_out(half, down, sg, su, sd, gain):
    experts, units, width = down.shape
    share = sg.shape[0] // experts
    per_step = experts // 2
    part = width // 2
    tail_rows = ceil_to(3 * share, PACKED_ROWS)
    strip = pl.BlockSpec((per_step * share, part), lambda i, h: (i, h[0]))
    return pl.pallas_call(
        functools.partial(pack_out_kernel, share),
        grid_spec=pltpu.PrefetchScalarGridSpec(
            num_scalar_prefetch=1,
            grid=(experts // per_step,),
            in_specs=[
                pl.BlockSpec((per_step, units, part), lambda i, h: (i, 0, h[0])),
                strip,
                strip,
                strip,
                pl.BlockSpec((1, part), lambda i, h: (0, h[0])),
            ],
            out_specs=pl.BlockSpec((per_step, units + tail_rows, part), lambda i, h: (i, 0, 0)),
            scratch_shapes=[pltpu.VMEM((tail_rows, part), jnp.float32)],
        ),
        out_shape=jax.ShapeDtypeStruct((experts, units + tail_rows, part), jnp.bfloat16),
        name="pack_out",
    )(half, down, sg, su, sd, gain)


def place_in_kernel(fs_count, tp_count, in_ref, out_ref):
    part = in_ref.shape[2]
    units = in_ref.shape[1] // 2
    lower = fs_count // 2
    columns = 2 * tp_count * units
    for f in range(fs_count):
        tiles = range(f * tp_count, (f + 1) * tp_count)
        gates = [in_ref[src, :units] for src in tiles]
        ups = [in_ref[src, units:] for src in tiles]
        rows = slice(f % lower * part, (f % lower + 1) * part)
        spot = f // lower * columns
        out_ref[rows, spot : spot + columns] = jnp.concatenate(gates + ups, axis=0).T


def place_in(landed, fs_count, tp_count):
    rows, part = landed.shape[1:]
    shape = (fs_count // 2 * part, 2 * tp_count * rows)
    return pl.pallas_call(
        functools.partial(place_in_kernel, fs_count, tp_count),
        in_specs=[IN_VMEM],
        out_specs=IN_VMEM,
        out_shape=jax.ShapeDtypeStruct(shape, jnp.bfloat16),
        compiler_params=SMALL_GRANT,
        name="place_in",
    )(landed)


def place_out_kernel(fs_count, tp_count, units, in_ref, out_ref):
    part = in_ref.shape[2]
    tail = in_ref.shape[1] - units
    strip_at = fs_count * units
    for f in range(fs_count):
        for t in range(tp_count):
            src = f * tp_count + t
            last = in_ref[src, units:]
            cols = slice(f * part, (f + 1) * part)
            out_ref[strip_at + t * tail : strip_at + (t + 1) * tail, cols] = last
            cols = slice(t * part, (t + 1) * part)
            out_ref[f * units : (f + 1) * units, cols] = in_ref[src, :units]


def place_out(landed, fs_count, tp_count, units):
    rows, part = landed.shape[1:]
    tail = rows - units
    out_rows = fs_count * units + tp_count * tail
    return pl.pallas_call(
        functools.partial(place_out_kernel, fs_count, tp_count, units),
        in_specs=[IN_VMEM],
        out_specs=IN_VMEM,
        out_shape=jax.ShapeDtypeStruct((out_rows, fs_count * part), jnp.bfloat16),
        compiler_params=SMALL_GRANT,
        name="place_out",
    )(landed)


def ffn_kernel(experts, gate_rows, strip_rows, share, tail, sources, own_ref, *refs):
    count = len(sources)
    blocks = refs[:count]
    own_in, peer_in = (refs[count], refs[count + 1]), (refs[count + 2], refs[count + 3])
    own_out, peer_out = (refs[count + 4], refs[count + 5]), (refs[count + 6], refs[count + 7])
    outs = refs[count + 8 :]
    rows, part = blocks[0].shape[0], own_out[0].shape[1]
    depth, columns = own_in[0].shape[0], 2 * gate_rows
    width = 2 * part
    down_rows = own_out[0].shape[0] - strip_rows
    tokens = [jnp.concatenate([b[:, n * part : (n + 1) * part] for b in blocks], axis=0) for n in range(2)]
    marks = [blocks[src][:, width:].astype(jnp.float32) for src, _ in sources]
    lane = lax.broadcasted_iota(jnp.int32, marks[0].shape, 1)
    span = marks[0].shape[1] // 2
    upper = lane >= span
    expert = lax.rem(lax.rem(lane, span), experts)

    def weight_of(n):
        parts = []
        for mark, (_, high) in zip(marks, sources):
            chosen = (expert == own_ref[n]) & (upper if high else ~upper)
            parts.append(jnp.sum(jnp.where(chosen, mark, 0.0), axis=1, keepdims=True))
        return jnp.concatenate(parts, axis=0)

    def regrouped(strips):
        side = strips.shape[0] // tail
        step = part // side
        bands = []
        for f in range(side):
            cols = slice(f * step, (f + 1) * step)
            bands.append(jnp.concatenate([strips[t * tail : (t + 1) * tail, cols] for t in range(side)], axis=1))
        return jnp.concatenate(bands, axis=0)

    def into(a, b):
        nt = (((1,), (1,)), ((), ()))
        return lax.dot_general(a, b, nt, preferred_element_type=jnp.float32)

    def onto(a, b):
        return jnp.dot(a, b, preferred_element_type=jnp.float32)

    hidden = []
    for n, mats in enumerate((own_in, peer_in)):
        weight = weight_of(n)
        both = 0.0
        for a, b in zip(tokens, mats):
            for k in range(part // depth):
                cols = slice(k * columns, (k + 1) * columns)
                both = both + onto(a[:, k * depth : (k + 1) * depth], b[:, cols])
        hidden.append((weight * silu(both[:, :gate_rows]) * both[:, gate_rows:]).astype(jnp.bfloat16))
    strip = 0.0
    for a, own, peer in zip(tokens, own_out, peer_out):
        strip = strip + into(a, jnp.concatenate([own[down_rows:], peer[down_rows:]], axis=0))
    place = lax.rem(lax.broadcasted_iota(jnp.int32, strip.shape, 1), tail)
    mine = (place >= 2 * share) & (place < 3 * share)
    gate = jnp.where(mine, pltpu.roll(strip, 2 * share, 1), 0.0)
    up = jnp.where(mine, pltpu.roll(strip, share, 1), 0.0)
    shared_hidden = (silu(gate) * up).astype(jnp.bfloat16)
    for n, (own, peer) in enumerate(zip(own_out, peer_out)):
        shared = jnp.concatenate([regrouped(own[down_rows:]), regrouped(peer[down_rows:])], axis=0)
        total = onto(hidden[0], own[:down_rows]) + onto(hidden[1], peer[:down_rows])
        total = (total + onto(shared_hidden, shared)).astype(jnp.bfloat16)
        for j in range(count):
            outs[j][:, n * part : (n + 1) * part] = total[j * rows : (j + 1) * rows]


def ffn(own, blocks, sources, mats, experts, sizes):
    rows, width = blocks[0].shape[0], 2 * mats[-1].shape[1]
    shape = jax.ShapeDtypeStruct((rows, width), jnp.bfloat16)
    return pl.pallas_call(
        functools.partial(ffn_kernel, experts, *sizes, sources),
        in_specs=[IN_SMEM] + [IN_VMEM] * (len(blocks) + len(mats)),
        out_specs=[IN_VMEM] * len(blocks),
        out_shape=[shape] * len(blocks),
        compiler_params=SMALL_GRANT,
        name="expert_ffn",
    )(own, *blocks, *mats)


def stage_kernel(*refs):
    count = len(refs) // 3
    copies = [pltpu.make_async_copy(refs[n], refs[count + n], refs[2 * count + n]) for n in range(count)]
    for copy in copies:
        copy.start()
    for copy in copies:
        copy.wait()


def stage(*arrays):
    return pl.pallas_call(
        stage_kernel,
        in_specs=[pl.BlockSpec(memory_space=pl.ANY)] * len(arrays),
        out_specs=[IN_VMEM] * len(arrays),
        out_shape=[pltpu.VMEM(a.shape, a.dtype) for a in arrays],
        scratch_shapes=[pltpu.SemaphoreType.DMA] * len(arrays),
        compiler_params=SMALL_GRANT,
        name="stage",
    )(*arrays)


def finish_kernel(tiles, half_ref, *refs):
    out_ref = refs[-1]
    rows, width = out_ref.shape
    part = width // tiles // 2
    swap = half_ref[0] != 0
    for n in range(2):
        mine = slice(n * (rows // 2), (n + 1) * (rows // 2))
        terms = refs[3 * n : 3 * n + 3]
        total = terms[0][...].astype(jnp.float32) + terms[1][...].astype(jnp.float32)
        total = (total + terms[2][...].astype(jnp.float32)).astype(jnp.bfloat16)
        for i in range(tiles):
            near = total[:, i * part : (i + 1) * part]
            far = total[:, width // 2 + i * part : width // 2 + (i + 1) * part]
            out_ref[mine, (2 * i) * part : (2 * i + 1) * part] = jnp.where(swap, far, near)
            out_ref[mine, (2 * i + 1) * part : (2 * i + 2) * part] = jnp.where(swap, near, far)


def finish(half, terms, tiles):
    rows, width = terms[0].shape
    return pl.pallas_call(
        functools.partial(finish_kernel, tiles),
        in_specs=[IN_SMEM] + [IN_VMEM] * len(terms),
        out_specs=IN_VMEM,
        out_shape=jax.ShapeDtypeStruct((2 * rows, width), jnp.bfloat16),
        compiler_params=SMALL_GRANT,
        name="finish",
    )(half, *terms)


def serve_kernel(fs_count, tp_count, half_ref, low_in, high_in, low_out, high_out, gate_ref, up_ref, down_ref):
    part = 2 * low_in.shape[0] // fs_count
    gate_rows = gate_ref.shape[1]
    swap = half_ref[0] != 0
    lower = fs_count // 2
    for f in range(fs_count):
        rows = slice(f % lower * part, (f % lower + 1) * part)
        for n, ref in enumerate((gate_ref, up_ref)):
            spot = (2 * (f // lower) + n) * gate_rows
            near, far = low_in[rows, spot : spot + gate_rows], high_in[rows, spot : spot + gate_rows]
            ref[(2 * f) * part : (2 * f + 1) * part, :] = jnp.where(swap, far, near)
            ref[(2 * f + 1) * part : (2 * f + 2) * part, :] = jnp.where(swap, near, far)
    rows = slice(0, down_ref.shape[0])
    part = low_out.shape[1] // tp_count
    for t in range(tp_count):
        cols = slice(t * part, (t + 1) * part)
        near, far = low_out[rows, cols], high_out[rows, cols]
        down_ref[:, (2 * t) * part : (2 * t + 1) * part] = jnp.where(swap, far, near)
        down_ref[:, (2 * t + 1) * part : (2 * t + 2) * part] = jnp.where(swap, near, far)


def serve(half, mats, fs_count, tp_count, gate_rows, down_rows):
    width = 2 * mats[-1].shape[1]
    tall = jax.ShapeDtypeStruct((width, gate_rows), jnp.bfloat16)
    return pl.pallas_call(
        functools.partial(serve_kernel, fs_count, tp_count),
        in_specs=[IN_SMEM] + [IN_VMEM] * 4,
        out_specs=[IN_VMEM] * 3,
        out_shape=[tall, tall, jax.ShapeDtypeStruct((down_rows, width), jnp.bfloat16)],
        compiler_params=SMALL_GRANT,
        name="serve",
    )(half, *mats)


def held_pack_kernel(gain_ref, sg_ref, su_ref, sd_ref, out_ref):
    units = sg_ref.shape[0]
    gain = gain_ref[...]
    out_ref[:units] = (sg_ref[...] * gain).astype(jnp.bfloat16)
    out_ref[units : 2 * units] = (su_ref[...] * gain).astype(jnp.bfloat16)
    out_ref[2 * units :] = sd_ref[...].astype(jnp.bfloat16)


def held_pack(gain, sg, su, sd):
    units, width = sg.shape
    return pl.pallas_call(
        held_pack_kernel,
        in_specs=[IN_VMEM] * 4,
        out_specs=IN_VMEM,
        out_shape=jax.ShapeDtypeStruct((3 * units, width), jnp.bfloat16),
        compiler_params=SMALL_GRANT,
        name="held_pack",
    )(gain, sg, su, sd)


def held_kernel(order_ref, *refs):
    tiles = refs[:-4]
    gate_ref, up_ref, down_ref, stage_ref = refs[-4:]
    units = tiles[0].shape[0] // 3
    count = len(tiles)
    width = tiles[0].shape[1]
    for r in range(count):
        spot = pl.multiple_of(order_ref[r] * units, units)
        for m in range(3):
            stage_ref[m, pl.ds(spot, units), :] = tiles[r][m * units : (m + 1) * units, :]
    gate_ref[...] = stage_ref[0].T
    up_ref[...] = stage_ref[1].T
    for t in range(count):
        down_ref[:, t * width : (t + 1) * width] = stage_ref[2, t * units : (t + 1) * units, :]


def held_tiles(order, tiles):
    count = len(tiles)
    units, width = tiles[0].shape[0] // 3, tiles[0].shape[1]
    tall = jax.ShapeDtypeStruct((width, count * units), jnp.bfloat16)
    return pl.pallas_call(
        held_kernel,
        in_specs=[IN_SMEM] + [IN_VMEM] * count,
        out_specs=[IN_VMEM] * 3,
        out_shape=[tall, tall, jax.ShapeDtypeStruct((units, count * width), jnp.bfloat16)],
        scratch_shapes=[pltpu.VMEM((3, count * units, width), jnp.bfloat16)],
        compiler_params=SMALL_GRANT,
        name="held_tiles",
    )(order, *tiles)


OUT_STREAMS = (("pa", 1, 0), ("nb", -1, 1), ("pb", 1, 1), ("na", -1, 0))


def gather_plan(
    tokens,
    route_ids,
    route_scores,
    norm_gain,
    expert_gate,
    expert_up,
    expert_down,
    shared_gate,
    shared_up,
    shared_down,
):
    fs_count = lax.axis_size("fs")
    tp_count = lax.axis_size("tp")
    experts = fs_count * tp_count
    ring = 2 * fs_count
    hops = fs_count
    half = lax.axis_index("grp").astype(jnp.int32)[None]
    tp_index = lax.axis_index("tp").astype(jnp.int32)
    me = lax.axis_index("fs").astype(jnp.int32) * tp_count + tp_index
    own = jnp.stack([me, me ^ 1])

    def spot(position, core):
        position = position % ring
        if position < fs_count:
            return position * tp_count + core
        return (ring - 1 - position) * tp_count + CORES + core

    def around(value, way):
        moves = [(spot(p, c), spot(p + way, c)) for p in range(ring) for c in range(CORES)]
        return lax.ppermute(value, ("fs", "tp"), moves)

    def across(value):
        return lax.ppermute(value, "tp", [(i, i ^ 1) for i in range(tp_count)])

    def sideways(value):
        return lax.ppermute(value, "tp", [(i, i ^ CORES) for i in range(tp_count)])

    gain = norm_gain[None, :]
    gate_t = jnp.transpose(expert_gate, (0, 2, 1))
    up_t = jnp.transpose(expert_up, (0, 2, 1))
    sg_t, su_t = shared_gate.T, shared_up.T
    units = gate_t.shape[1]
    share = sg_t.shape[0] // experts
    gate_rows, down_rows = tp_count * units, fs_count * units
    packed = pack_in(half, gate_t, up_t, gain)
    landed = lax.all_to_all(packed, ("fs", "tp"), split_axis=0, concat_axis=0, tiled=True)
    low_in = place_in(landed, fs_count, tp_count)
    packed = pack_out(half, expert_down, sg_t, su_t, shared_down, gain)
    tail = packed.shape[1] - units
    landed = lax.all_to_all(packed, ("fs", "tp"), split_axis=0, concat_axis=0, tiled=True)
    low_out = place_out(landed, fs_count, tp_count, units)
    high_in = lax.ppermute(low_in, "grp", [(0, 1), (1, 0)])
    high_out = lax.ppermute(low_out, "grp", [(0, 1), (1, 0)])
    peer_low_in, peer_low_out = across(low_in), across(low_out)
    peer_high_in = across(high_in)
    peer_high_out = across(high_out)
    near_in, peer_low_in, near_out, peer_low_out = stage(low_in, peer_low_in, low_out, peer_low_out)
    high_in, peer_high_in = stage(high_in, peer_high_in)
    high_out, peer_high_out = stage(high_out, peer_high_out)
    mats = (near_in, high_in, peer_low_in, peer_high_in, near_out, high_out, peer_low_out, peer_high_out)

    seen = {}
    pair = norm_rows(half, tokens, route_ids, route_scores, experts, fs_count)
    for name, _, n in OUT_STREAMS:
        seen[name] = [pair[n]]
    for s in range(1, hops + 1):
        for name, way, _ in OUT_STREAMS:
            if s < hops or name in ("pa", "nb"):
                seen[name].append(around(seen[name][-1], way))

    sizes = (gate_rows, tp_count * tail, share, tail)
    made = {name: {} for name in seen}
    for s in range(hops, 0, -1):
        keys = [(name, s) for name, _, _ in OUT_STREAMS if s < len(seen[name])]
        if s == 1:
            keys += [("pa", 0), ("pb", 0)]
        holders = {name: ("pa" if s == hops else name[0] + "a") for name, _, _ in OUT_STREAMS}
        sources = tuple((keys.index((holders[name], d)), name[1] == "b") for name, d in keys)
        outs = ffn(own, [seen[name][d] for name, d in keys], sources, mats, experts, sizes)
        for (name, d), out in zip(keys, outs):
            made[name][d] = out

    ended = {}
    for name, way, _ in OUT_STREAMS:
        deepest = max(made[name])
        moving = made[name][deepest]
        for d in range(deepest - 1, -1, -1):
            moving = around(moving, -way)
            if d > 0:
                moving = (moving.astype(jnp.float32) + made[name][d].astype(jnp.float32)).astype(jnp.bfloat16)
        ended[name] = moving
    terms = (made["pa"][0], ended["pa"], ended["na"], made["pb"][0], ended["pb"], ended["nb"])
    mixed = finish(half, terms, tp_count)

    served_gate, served_up, served_down = serve(
        half, (near_in, high_in, near_out, high_out), fs_count, tp_count, gate_rows, down_rows
    )

    tile = held_pack(gain, sg_t, su_t, shared_down)
    tiles = [tile, sideways(tile)]
    tiles += [across(tiles[0]), across(tiles[1])]
    order = jnp.stack([tp_index, tp_index ^ CORES, tp_index ^ 1, tp_index ^ (CORES + 1)])
    held_gate, held_up, held_down = held_tiles(order, tiles)
    return (mixed, served_gate[None], served_up[None], served_down[None], held_gate, held_up, held_down)


def gathers(fs_count, tp_count, picks, groups):
    square = fs_count == tp_count == 2 * CORES
    return fs_count * tp_count <= 2 * picks and groups == 2 and square


def on_device(tokens, route_ids, *others):
    fs_count, tp_count = lax.axis_size("fs"), lax.axis_size("tp")
    if gathers(fs_count, tp_count, route_ids.shape[1], lax.axis_size("grp")):
        return gather_plan(tokens, route_ids, *others)
    return exchange_plan(tokens, route_ids, *others)


def solution(mesh):
    return jax.shard_map(
        on_device,
        mesh=mesh,
        in_specs=(
            P(("grp", "fs", "tp"), None),
            P(("grp", "fs", "tp"), None),
            P(("grp", "fs", "tp"), None),
            P("fs"),
            P(None, "fs", "tp"),
            P(None, "fs", "tp"),
            P(None, "fs", "tp"),
            P("fs", "tp"),
            P("fs", "tp"),
            P("fs", "tp"),
        ),
        out_specs=(
            P(("grp", "fs", "tp"), None),
            P(("grp", "fs", "tp"), None, None),
            P(("grp", "fs", "tp"), None, None),
            P(("grp", "fs", "tp"), None, None),
            P(("grp", "fs"), None),
            P(("grp", "fs"), None),
            P(("grp", "fs"), None),
        ),
        check_vma=False,
    )
```
